32 devices in a mesh: grp: 2 (over y), ep: 4 (over z), tp: 4 (over x, core).
Axes of the slice: x: 2, y: 2, z: 4, core: 2. Of those that a mesh axis runs over, the one named last changes fastest.
Arguments:
- queries: bfloat16 [4096, 768], P(('grp', 'ep'), 'tp'), parts along dimension 0, may hold values from -6 to 6
- key_value: bfloat16 [4096, 4, 128], P(('grp', 'ep'), 'tp'), parts along dimension 0, may hold values from -6 to 6
- key_bias: bfloat16 [4, 4096], P('tp', ('grp', 'ep')), parts along dimension 1, may hold values from -20 to 0
- out_weight: bfloat16 [768, 2048], P('tp'), may hold values from -0.75 to 0.75
- expert_input: bfloat16 [4096, 2048], P(('grp', 'ep', 'tp')), parts along dimension 0, may hold values from -6 to 6
- norm_gain: float32 [2048], replicated, may hold values from 0.1 to 1.9
- routes: int32 [4096, 4], P(('grp', 'ep', 'tp')), parts along dimension 0, may hold values from 0 to 15, as said below
- route_weights: float32 [4096, 4], P(('grp', 'ep', 'tp')), parts along dimension 0, may hold values from 0.2 to 1
- gate_weight: bfloat16 [16, 2048, 512], P(('ep', 'tp')), may hold values from -0.125 to 0.125
- up_weight: bfloat16 [16, 2048, 512], P(('ep', 'tp')), may hold values from -0.125 to 0.125
- down_weight: bfloat16 [16, 512, 2048], P(('ep', 'tp')), may hold values from -0.25 to 0.25
- shared_gate: bfloat16 [2048, 256], replicated, may hold values from -0.125 to 0.125
- shared_up: bfloat16 [2048, 256], replicated, may hold values from -0.125 to 0.125
- shared_down: bfloat16 [256, 2048], replicated, may hold values from -0.375 to 0.375
Outputs:
- mixer_output: bfloat16 [4096, 2048], P(('grp', 'ep', 'tp')), parts along dimension 0
- expert_output: bfloat16 [4096, 2048], P(('grp', 'ep', 'tp')), parts along dimension 0
The draws below stay inside these ranges and needn't reach their ends.
There are 2 independent parts, one for each index of `grp`. The reference program is written for one: setup_inputs(seed, part) draws one part's arguments, and reference() takes and returns one part's arrays. A program takes and returns all parts, laid end to end along the dimension named above; an argument that names none is the same for every part. Nothing has to cross between parts.
Inputs may be any that keep to these rules, and one draw needn't show every extreme that they name: `routes`: each row names 4 different experts. Among the 128 rows of one device no expert is named more than 48 times, and in every draw one expert is named exactly 48 times in the rows of every device.
All inputs are finite; a program needn't handle non-finite values.
Results may differ from the reference program's by a relative error of at most 0.009.
Values may be sent and summed in bfloat16 or wider, within the bound.
A program may use at most 128 MiB of HBM per device.

```python
import math
import jax
import jax.numpy as jnp
import numpy as np
from jax import lax

D = 2048
HD = 64
HEADS = 12
KEY_HEAD_COUNT = 4
EFF = 512
SFF = 256
TOPK = 4
TOK = 128
SPAN = 512
DEVSEQ = 4
SEQUENCE_LENGTH = 2048
TOTAL_POSITIONS = 2048
TOKENS = 2048
EXPERTS = 16
CAP = 48
HOT = 2
N_TP = 4


def draw_routes(key, part):
    key_hot = jax.random.fold_in(key, 11)
    key_order = jax.random.fold_in(key, 12)
    key_rows = jax.random.fold_in(key, 13)
    sources = TOKENS // TOK
    hot_expert = jax.random.randint(key_hot, (), 0, EXPERTS, dtype=jnp.int32)
    ordinal = jnp.broadcast_to(jnp.arange(EXPERTS, dtype=jnp.int32), (sources, EXPERTS))
    orders = jax.random.permutation(key_order, ordinal, axis=1, independent=True)
    hot_place = jnp.argmax(orders == hot_expert, axis=1)
    columns = jnp.arange(EXPERTS, dtype=jnp.int32)[None, :]
    leading = orders[:, :1]
    orders = jnp.where(columns == 0, hot_expert, jnp.where(columns == hot_place[:, None], leading, orders))
    remaining = TOK * TOPK - HOT * CAP
    others = EXPERTS - HOT
    counts = np.array([CAP] * HOT + [remaining // others + (1 if index < remaining % others else 0) for index in range(others)])
    rank_list = np.repeat(np.arange(EXPERTS), counts)
    tickets = orders[:, rank_list]
    laid_out = jnp.transpose(tickets.reshape(sources, TOPK, TOK), (0, 2, 1))
    row_ordinal = jnp.broadcast_to(jnp.arange(TOK, dtype=jnp.int32), (sources, TOK))
    row_orders = jax.random.permutation(key_rows, row_ordinal, axis=1, independent=True)
    shuffled = jnp.take_along_axis(laid_out, jnp.broadcast_to(row_orders[:, :, None], laid_out.shape), axis=1)
    return shuffled.reshape(TOKENS, TOPK).astype(jnp.int32)


def draw_key_bias(key, part):
    ranking = jax.random.permutation(jax.random.fold_in(key, 21), KEY_HEAD_COUNT)
    fast_count = KEY_HEAD_COUNT // 2
    is_fast = ranking < fast_count
    drawn_version = jnp.where(is_fast, -jnp.log(40.0), -jnp.log(float(SEQUENCE_LENGTH)) - 1.0)[:, None]
    jaggedness = jax.random.uniform(jax.random.fold_in(key, 22), (KEY_HEAD_COUNT, TOTAL_POSITIONS), jnp.float32, -0.5, 0.5)
    block_by_block = jax.random.uniform(jax.random.fold_in(key, 23), (KEY_HEAD_COUNT, TOTAL_POSITIONS // SPAN), jnp.float32, -0.7, 0.7)
    block_by_block = jnp.repeat(block_by_block, SPAN, axis=1)
    spike_events = jax.random.randint(jax.random.fold_in(key, 24), (KEY_HEAD_COUNT, TOTAL_POSITIONS), 0, SEQUENCE_LENGTH) < 3
    spike_height = jax.random.uniform(jax.random.fold_in(key, 25), (KEY_HEAD_COUNT, TOTAL_POSITIONS), jnp.float32, -1.2, -0.3)
    return jnp.where(spike_events, spike_height, drawn_version + jaggedness + block_by_block).astype(jnp.bfloat16)


def level_of(stream_key, extent, split, smallest, high):
    gain, own = 1.0, jax.random.fold_in(stream_key, 6)
    for dim, blocks in split:
        heights = jnp.exp(jax.random.uniform(jax.random.fold_in(own, dim), (blocks,), jnp.float32, smallest / len(split), high / len(split)))
        gain = gain * jnp.repeat(heights, extent[dim] // blocks).reshape([-1 if axis == dim else 1 for axis in range(len(extent))])
    return gain


def gaussian(key, shape, spread, limit, shards=(), kind=jnp.bfloat16):
    drawn = spread * jax.random.normal(key, shape, jnp.float32)
    if shards:
        drawn = drawn * level_of(key, shape, shards, -0.22, 0.18)
    return jnp.clip(drawn, -limit, limit).astype(kind)


def setup_inputs(seed: int = 0, part: int = 0) -> dict:
    keys = jax.random.split(jax.random.key(seed), 15)
    part_splits = jax.random.split(jax.random.fold_in(keys[14], part), 15)
    return {
        "queries": gaussian(part_splits[0], (TOTAL_POSITIONS, HEADS * HD), 1.0, 6.0, ((0, 4), (1, 4))),
        "key_value": gaussian(part_splits[1], (TOTAL_POSITIONS, KEY_HEAD_COUNT, 2 * HD), 1.0, 6.0, ((0, 4), (1, 4))),
        "key_bias": draw_key_bias(jax.random.fold_in(jax.random.fold_in(keys[14], part), 71), part),
        "out_weight": gaussian(keys[3], (HEADS * HD, D), HD ** -0.5, 0.75, ((0, 4),)),
        "expert_input": gaussian(part_splits[4], (TOKENS, D), 1.0, 6.0, ((0, 16),)),
        "norm_gain": jnp.clip(1.0 + 0.18 * jax.random.normal(keys[5], (D,), jnp.float32), 0.1, 1.9),
        "routes": draw_routes(jax.random.fold_in(jax.random.fold_in(keys[14], part), 71), part),
        "route_weights": jnp.clip(jnp.exp(math.log(1.0) - 1.609438 * jax.random.uniform(part_splits[7], (TOKENS, TOPK), jnp.float32) ** level_of(part_splits[7], (TOKENS, TOPK), ((0, 16),), -0.2, 0.2)), 0.2, 1.0),
        "gate_weight": gaussian(keys[8], (EXPERTS, D, EFF), D ** -0.5, 0.125, ((0, 16),)),
        "up_weight": gaussian(keys[9], (EXPERTS, D, EFF), D ** -0.5, 0.125, ((0, 16),)),
        "down_weight": gaussian(keys[10], (EXPERTS, EFF, D), EFF ** -0.5, 0.25, ((0, 16),)),
        "shared_gate": gaussian(keys[11], (D, SFF), D ** -0.5, 0.125),
        "shared_up": gaussian(keys[12], (D, SFF), D ** -0.5, 0.125),
        "shared_down": gaussian(keys[13], (SFF, D), SFF ** -0.5, 0.375),
    }


def piece_update(running, query_rows, key_rows, value_rows, key_offset, allowed):
    totals, kept_sum = running
    logits = jnp.einsum('sgrd,kgd->grsk', query_rows.astype(jnp.float32), key_rows.astype(jnp.float32)) * 0.125
    logits = logits + key_offset.astype(jnp.float32)[:, None, None, :]
    log_keep = jnp.where(allowed, -jax.nn.softplus(logits), 0.0)
    log_after = lax.cumsum(log_keep, axis=3, reverse=True) - log_keep
    weights = jnp.where(allowed, jnp.exp(jax.nn.log_sigmoid(logits) + log_after + kept_sum[..., None]), 0.0)
    weights = weights.astype(jnp.bfloat16)
    totals = totals + jnp.einsum('grsk,kgd->grsd', weights.astype(jnp.float32), value_rows.astype(jnp.float32))
    return (totals, kept_sum + lax.optimization_barrier(jnp.sum(log_keep, axis=3)))

def mixer_reference(queries, key_value, key_bias, out_weight):
    per_group = HEADS // KEY_HEAD_COUNT
    block_count = TOTAL_POSITIONS // SPAN
    query_blocks = queries.reshape(block_count, SPAN, KEY_HEAD_COUNT, per_group, HD)
    key_blocks = key_value[..., :HD].reshape(block_count, SPAN, KEY_HEAD_COUNT, HD)
    value_blocks = key_value[..., HD:].reshape(block_count, SPAN, KEY_HEAD_COUNT, HD)
    bias_blocks = jnp.transpose(key_bias.reshape(KEY_HEAD_COUNT, block_count, SPAN), (1, 0, 2))
    positions = jnp.arange(SPAN, dtype=jnp.int32)
    strict_mask = positions[None, :] < positions[:, None]
    full_mask = jnp.ones((SPAN, SPAN), dtype=bool)

    def one_block(block_index):
        query_rows = query_blocks[block_index]
        initial = (jnp.zeros((KEY_HEAD_COUNT, per_group, SPAN, HD), jnp.float32), jnp.zeros((KEY_HEAD_COUNT, per_group, SPAN), jnp.float32))
        running = piece_update(initial, query_rows, key_blocks[block_index], value_blocks[block_index], bias_blocks[block_index], strict_mask)

        def advance(distance, current):
            source = block_index - distance
            return piece_update(current, query_rows, key_blocks[source], value_blocks[source], bias_blocks[source], full_mask)
        chain_place = jnp.minimum((block_index + 2) % DEVSEQ, block_index)
        running = lax.fori_loop(1, chain_place + 1, advance, running)
        return running[0].astype(jnp.bfloat16)
    attended = lax.map(one_block, jnp.arange(block_count, dtype=jnp.int32))
    weight_blocks = out_weight.reshape(KEY_HEAD_COUNT, per_group, HD, D)
    group_heads = KEY_HEAD_COUNT // N_TP
    summed = jnp.zeros((block_count, SPAN, D), jnp.float32)
    for group_index in range(N_TP):
        part_rows = attended[:, group_index * group_heads:(group_index + 1) * group_heads].astype(jnp.float32)
        part_weight = weight_blocks[group_index * group_heads:(group_index + 1) * group_heads].astype(jnp.float32)
        group_terms = jnp.einsum('bgrsd,grde->bse', part_rows, part_weight).astype(jnp.bfloat16)
        summed = summed + group_terms.astype(jnp.float32)
    return summed.reshape(TOTAL_POSITIONS, D).astype(jnp.bfloat16)

def experts_reference(expert_input, norm_gain, routes, route_weights, gate_weight, up_weight, down_weight, shared_gate, shared_up, shared_down):
    widened = expert_input.astype(jnp.float32)
    normed = (widened * lax.rsqrt(lax.optimization_barrier(jnp.mean(widened * widened, axis=-1, keepdims=True)) + 1e-06) * norm_gain).astype(jnp.bfloat16)
    sources = TOKENS // TOK
    pair_count = TOK * TOPK
    block_routes = routes.reshape(sources, pair_count)
    one_hot = (block_routes[..., None] == jnp.arange(EXPERTS, dtype=jnp.int32)).astype(jnp.int32)
    slot_index = lax.optimization_barrier(jnp.sum((jnp.cumsum(one_hot, axis=1) - one_hot) * one_hot, axis=2))
    placing = (block_routes * sources + jnp.arange(sources, dtype=jnp.int32)[:, None]) * CAP + slot_index
    empty_pair = TOKENS * TOPK
    table = jnp.full((EXPERTS * sources * CAP,), empty_pair, jnp.int32)
    table = table.at[placing.reshape(-1)].set(jnp.arange(empty_pair, dtype=jnp.int32))
    table = table.reshape(EXPERTS, sources * CAP)
    padded_rows = jnp.concatenate([normed, jnp.zeros((1, D), jnp.bfloat16)], axis=0)
    padded_weights = jnp.concatenate([route_weights.reshape(-1), jnp.zeros((1,), jnp.float32)], axis=0)

    def expert_step(accumulated, inputs):
        picks, gate_one, up_one, down_one = inputs
        owners = picks // TOPK
        chosen = padded_rows[owners]
        gate_part = jnp.dot(chosen, gate_one, preferred_element_type=jnp.float32)
        up_part = jnp.dot(chosen, up_one, preferred_element_type=jnp.float32)
        hidden = (jax.nn.silu(gate_part) * up_part).astype(jnp.bfloat16)
        result = jnp.dot(hidden, down_one, preferred_element_type=jnp.float32).astype(jnp.bfloat16)
        scaled = result.astype(jnp.float32) * padded_weights[picks][:, None]
        return (accumulated.at[owners].add(scaled, mode='drop'), None)
    routed, _ = lax.scan(expert_step, jnp.zeros((TOKENS, D), jnp.float32), (table, gate_weight, up_weight, down_weight))
    shared_hidden = (jax.nn.silu(jnp.dot(normed, shared_gate, preferred_element_type=jnp.float32)) * jnp.dot(normed, shared_up, preferred_element_type=jnp.float32)).astype(jnp.bfloat16)
    shared_term = jnp.dot(shared_hidden, shared_down, preferred_element_type=jnp.float32)
    return (routed + shared_term).astype(jnp.bfloat16)

def reference(queries, key_value, key_bias, out_weight, expert_input, norm_gain, routes, route_weights, gate_weight, up_weight, down_weight, shared_gate, shared_up, shared_down):
    mixer_output = mixer_reference(queries, key_value, key_bias, out_weight)
    expert_output = experts_reference(expert_input, norm_gain, routes, route_weights, gate_weight, up_weight, down_weight, shared_gate, shared_up, shared_down)
    return (mixer_output, expert_output)
```

```python
import jax
import jax.numpy as jnp
from jax import lax
from jax.experimental import pallas as pl
from jax.experimental.pallas import tpu as pltpu
from jax.sharding import PartitionSpec as P

MESH = pl.DeviceIdType.MESH
F32 = jnp.float32
BF16 = jnp.bfloat16


def passed_along(block, axis, distance):
    devices = range(lax.axis_size(axis))
    route = [(i - distance, i) for i in devices if i - distance in devices]
    return lax.ppermute(block, axis, route)


def attention_tile(q, k, v, bias, upper, kept, masked):
    z = lax.dot_general(q, k, (((1,), (1,)), ((), ())), preferred_element_type=F32) * 0.125 + bias
    tail = jnp.log(1.0 + jnp.exp(-jnp.abs(z)))
    log_sig = jnp.minimum(z, 0.0) - tail
    keep = -(jnp.maximum(z, 0.0) + tail)
    if masked:
        rows = lax.broadcasted_iota(jnp.int32, z.shape, 0)
        columns = lax.broadcasted_iota(jnp.int32, z.shape, 1)
        allowed = columns < rows
        keep = jnp.where(allowed, keep, 0.0)
    high = keep.astype(BF16)
    low = (keep - high.astype(F32)).astype(BF16)
    after = jnp.dot(high, upper, preferred_element_type=F32)
    after = after + jnp.dot(low, upper, preferred_element_type=F32)
    weight = jnp.exp(log_sig + after + kept)
    if masked:
        weight = jnp.where(allowed, weight, 0.0)
    part = jnp.dot(weight.astype(BF16), v, preferred_element_type=F32)
    return part, kept + jnp.sum(keep, axis=1, keepdims=True)


def attention_kernel(place_ref, q_ref, kv_ref, bias_ref, out_ref, total, kept):
    span, head_dim = q_ref.shape[1:]
    spans = kv_ref.shape[0]
    size = min(span, 256)
    tiles = span // size
    rows = lax.broadcasted_iota(jnp.int32, (size, size), 0)
    columns = lax.broadcasted_iota(jnp.int32, (size, size), 1)
    upper = jnp.where(rows > columns, 1.0, 0.0).astype(BF16)

    def tile(distance, i, j, masked, state):
        there = pl.ds(j * size, size)
        part, after = attention_tile(
            q_ref[0, i * size : (i + 1) * size, :],
            kv_ref[distance, 0, there, :head_dim],
            kv_ref[distance, 0, there, head_dim:],
            bias_ref[distance, 0, :, there].astype(F32),
            upper,
            state[1],
            masked,
        )
        return state[0] + part, after

    for i in range(tiles):
        state = (jnp.zeros((size, head_dim), F32), jnp.zeros((size, 1), F32))
        for j in range(i, -1, -1):
            state = tile(0, i, j, j == i, state)
        total[i] = state[0]
        kept[i] = jnp.broadcast_to(state[1], kept.shape[1:])
    for distance in range(1, spans):

        @pl.when(distance <= place_ref[0])
        def _():
            for i in range(tiles):
                state = (total[i], kept[i, :, :1])
                for j in range(tiles - 1, -1, -1):
                    state = tile(distance, i, j, False, state)
                total[i] = state[0]
                kept[i] = jnp.broadcast_to(state[1], kept.shape[1:])

    for i in range(tiles):
        out_ref[0, i * size : (i + 1) * size, :] = total[i].astype(out_ref.dtype)


def attend(queries, key_value, key_bias):
    span, key_groups, pair_width = key_value.shape
    head_dim = pair_width // 2
    heads = queries.shape[1] // head_dim
    per_group = heads // key_groups
    axis_size = lax.axis_size("ep")
    chain_length = axis_size // max(1, axis_size // 4)
    place = lax.axis_index("ep")
    chain_place = jnp.minimum((place + 2) % chain_length, place)
    furthest = max(min((p + 2) % chain_length, p) for p in range(axis_size))
    packed = jnp.concatenate([key_value.reshape(-1, pair_width), key_bias.reshape(-1, pair_width)])
    visiting = [packed]
    for _ in range(furthest):
        visiting.append(passed_along(visiting[-1], "ep", 1))
    visiting = jnp.stack(visiting)
    keys = visiting[:, : span * key_groups].reshape(-1, span, key_groups, pair_width)
    keys = keys.transpose(0, 2, 1, 3)
    biases = visiting[:, span * key_groups :].reshape(-1, key_groups, 1, span)
    size = min(span, 256)
    attended = pl.pallas_call(
        attention_kernel,
        grid=(heads,),
        out_shape=jax.ShapeDtypeStruct((heads, span, head_dim), BF16),
        in_specs=[
            pl.BlockSpec(memory_space=pltpu.SMEM),
            pl.BlockSpec((1, span, head_dim), lambda h: (h, 0, 0)),
            pl.BlockSpec((furthest + 1, 1, span, pair_width), lambda h: (0, h // per_group, 0, 0)),
            pl.BlockSpec((furthest + 1, 1, 1, span), lambda h: (0, h // per_group, 0, 0)),
        ],
        out_specs=pl.BlockSpec((1, span, head_dim), lambda h: (h, 0, 0)),
        scratch_shapes=[
            pltpu.VMEM((span // size, size, head_dim), F32),
            pltpu.VMEM((span // size, size, 128), F32),
        ],
        name="attention",
        cost_estimate=pl.CostEstimate(flops=4 * 10**9, bytes_accessed=10**6, transcendentals=0),
    )(
        chain_place.reshape(1),
        queries.reshape(span, heads, head_dim).transpose(1, 0, 2),
        keys,
        biases,
    )
    return attended.transpose(1, 0, 2).reshape(span, heads * head_dim)


def project(attended, out_weight):
    return jnp.dot(attended, out_weight, preferred_element_type=F32).astype(BF16)


def exchange_kernel(
    capacity,
    terms_ref,
    normed_ref,
    meta_ref,
    shared_gate,
    shared_up,
    shared_down,
    gate_hbm,
    up_hbm,
    down_hbm,
    mixer_ref,
    expert_ref,
    gathered,
    meta,
    gate_v,
    up_v,
    down_v,
    chosen,
    shared,
    sums,
    from_sibling,
    from_side,
    from_line,
    mixer_sibling,
    mixer_side,
    mixer_sum,
    load_sem,
    meta_send,
    meta_recv,
    zs_send,
    zs_recv,
    x_send,
    x_recv,
    s_send,
    s_recv,
    rz_send,
    rz_recv,
    rx_send,
    rx_recv,
    rs_send,
    rs_recv,
    m_send,
    m_recv,
):
    count = lax.axis_size("ep")
    width = normed_ref.shape[1]
    tokens = normed_ref.shape[0]
    half = width // 2
    z = lax.axis_index("ep")
    t = lax.axis_index("tp")
    x, c = t // 2, t % 2
    ox, oc = 1 - x, 1 - c
    side, sibling = ox * 2 + c, x * 2 + oc
    group = count * 4
    me = z * 4 + t

    loads = [
        pltpu.make_async_copy(a, b, load_sem.at[i])
        for i, (a, b) in enumerate(((gate_hbm, gate_v), (up_hbm, up_v), (down_hbm, down_v)))
    ]
    own_load = pltpu.make_async_copy(normed_ref, gathered.at[z, x, c], load_sem.at[3])
    own_meta = pltpu.make_async_copy(meta_ref.at[me], meta.at[me], load_sem.at[4])
    own_load.start()
    own_meta.start()

    barrier = pltpu.get_barrier_semaphore()
    for step in range(1, group):
        other = (me + step) % group
        pl.semaphore_signal(
            barrier, 1, device_id={"ep": other // 4, "tp": other % 4}, device_id_type=MESH
        )
    pl.semaphore_wait(barrier, group - 1)

    def copy(src, dst, send, recv, ep, tp):
        return pltpu.make_async_remote_copy(
            src_ref=src,
            dst_ref=dst,
            send_sem=send,
            recv_sem=recv,
            device_id={"ep": ep, "tp": tp},
            device_id_type=MESH,
        )

    own_load.wait()
    own_meta.wait()

    def part(zz, xx, cc, h):
        return gathered.at[zz, xx, cc, :, pl.ds(h * half, half)]

    def line(up, kind, zz):
        block = part(zz, ox if kind == 1 else x, c, 1 if kind == 2 else 0)
        return copy(
            block,
            block,
            zs_send.at[0 if up else 1, kind, zz],
            zs_recv.at[kind, zz],
            z + (1 if up else -1),
            t,
        )

    def across(slot, zz):
        block = part(zz, x, c, 0 if slot == 0 else 1)
        index = 0 if slot == 0 else 1 + zz
        return copy(block, block, x_send.at[index], x_recv.at[index], z, side)

    def across_in(slot, zz):
        block = part(zz, ox, c, 0 if slot == 0 else 1)
        index = 0 if slot == 0 else 1 + zz
        return copy(block, block, x_send.at[index], x_recv.at[index], z, side)

    def share(zz, xx, h):
        block = part(zz, xx, c, h)
        return copy(block, block, s_send.at[zz, xx, h], s_recv.at[zz, xx, h], z, sibling)

    def share_in(zz, xx, h):
        block = part(zz, xx, oc, h)
        return copy(block, block, s_send.at[zz, xx, h], s_recv.at[zz, xx, h], z, sibling)

    def meta_copy(step):
        other = (me + step) % group
        return copy(
            meta_ref.at[other],
            meta.at[me],
            meta_send.at[step - 1],
            meta_recv.at[step - 1],
            other // 4,
            other % 4,
        )

    def meta_in(step):
        other = (me + group - step) % group
        return copy(
            meta_ref.at[other],
            meta.at[other],
            meta_send.at[step - 1],
            meta_recv.at[step - 1],
            other // 4,
            other % 4,
        )

    can_up, can_down = z + 1 < count, z >= 1

    across(0, z).start()
    for kind in (0, 2):

        @pl.when(can_up)
        def _():
            line(True, kind, z).start()

        @pl.when(can_down)
        def _():
            line(False, kind, z).start()

    across(1, z).start()
    for step in range(1, group):
        meta_copy(step).start()
    share(z, x, 0).start()
    share(z, x, 1).start()
    for load in loads:
        load.start()

    def mixer_pair(xx):
        return copy(
            terms_ref.at[xx, oc],
            mixer_sibling.at[xx],
            m_send.at[xx],
            m_recv.at[xx],
            z,
            sibling,
        )

    for xx in range(2):
        mixer_pair(xx).start()

    across_in(0, z).wait_recv()

    @pl.when(can_up)
    def _():
        line(True, 1, z).start()

    @pl.when(can_down)
    def _():
        line(False, 1, z).start()

    share(z, ox, 0).start()

    hidden_gate = jnp.dot(normed_ref[...], shared_gate[...], preferred_element_type=F32)
    hidden_up = jnp.dot(normed_ref[...], shared_up[...], preferred_element_type=F32)
    shared_hidden = (hidden_gate / (1.0 + jnp.exp(-hidden_gate)) * hidden_up).astype(BF16)
    shared[...] = jnp.dot(shared_hidden, shared_down[...], preferred_element_type=F32)

    for distance in range(1, count):
        below, above = z - distance, z + distance

        def arrive(kind, zz, going_up, further):
            line(going_up, kind, zz).wait_recv()

            @pl.when(further)
            def _():
                line(going_up, kind, zz).start()

            if kind == 2:
                across(1, zz).start()
            share(zz, ox if kind == 1 else x, 1 if kind == 2 else 0).start()

        for kind in (0, 2, 1):

            @pl.when(below >= 0)
            def _():
                arrive(kind, below, True, can_up)

            @pl.when(above < count)
            def _():
                arrive(kind, above, False, can_down)

    for xx in range(2):
        mixer_pair(xx).wait()
    mixer_sum[...] = (
        terms_ref[ox, c].astype(F32) + mixer_sibling[ox].astype(F32)
    ).astype(BF16)
    mixer_move = copy(mixer_sum, mixer_side, m_send.at[2], m_recv.at[2], z, side)
    mixer_move.start()

    for step in range(count):
        zz = (z + step) % count
        across_in(1, zz).wait_recv()
        share(zz, ox, 1).start()
    for step in range(1, group):
        meta_in(step).wait_recv()
    for zz in range(count):
        for xx in range(2):
            for h in range(2):
                share_in(zz, xx, h).wait_recv()
    for load in loads:
        load.wait()

    batch = chosen.shape[0] // capacity
    slots = lax.broadcasted_iota(jnp.int32, (capacity, tokens), 0).astype(F32)

    def picker(source):
        return jnp.where(meta[source, 1:2, :] == slots, 1.0, 0.0)

    @pl.loop(0, group // batch)
    def _(turn):
        for i in range(batch):
            source = turn * batch + i
            block = gathered[source // 4, (source % 4) // 2, source % 2]
            chosen[i * capacity : (i + 1) * capacity, :] = jnp.dot(
                picker(source).astype(BF16), block, preferred_element_type=F32
            ).astype(BF16)
        gate = jnp.dot(chosen[...], gate_v[...], preferred_element_type=F32)
        up = jnp.dot(chosen[...], up_v[...], preferred_element_type=F32)
        hidden = (gate / (1.0 + jnp.exp(-gate)) * up).astype(BF16)
        for i in range(batch):
            source = turn * batch + i
            pick = picker(source)
            scale = jnp.sum(pick * meta[source, 0:1, :], axis=1, keepdims=True)
            rows = jnp.dot(
                hidden[i * capacity : (i + 1) * capacity, :],
                down_v[...],
                preferred_element_type=F32,
            )
            rows = (rows * scale).astype(BF16)
            sums[source // 4, (source % 4) // 2, source % 2] = lax.dot_general(
                pick.astype(BF16), rows, (((0,), (0,)), ((), ())), preferred_element_type=F32
            ).astype(BF16)

    def pair(zz, xx):
        return copy(
            sums.at[zz, xx, oc],
            from_sibling.at[zz, xx],
            rs_send.at[zz, xx],
            rs_recv.at[zz, xx],
            z,
            sibling,
        )

    def half_ref(zz, xx, h):
        return sums.at[zz, xx, c, :, pl.ds(h * half, half)]

    def side_move(zz):
        return copy(
            half_ref(zz, ox, 1), from_side.at[1 + zz], rx_send.at[1 + zz], rx_recv.at[1 + zz], z, side
        )

    def last_move():
        return copy(half_ref(z, ox, 0), from_side.at[0], rx_send.at[0], rx_recv.at[0], z, side)

    def back(up, kind, zz):
        return copy(
            half_ref(zz, ox if kind == 1 else x, 1 if kind == 2 else 0),
            from_line.at[0 if up else 1, kind, zz],
            rz_send.at[kind, zz],
            rz_recv.at[0 if up else 1, kind, zz],
            z + (1 if up else -1),
            t,
        )

    def add(ref, other):
        ref[...] = (ref[...].astype(F32) + other[...].astype(F32)).astype(BF16)

    order = []
    for step in range(count):
        order.append((z + count // 2 + step) % count)
    for zz in order:
        for xx in (ox, x):
            pair(zz, xx).start()
    for zz in order:
        for xx in (ox, x):
            pair(zz, xx).wait_recv()
            add(sums.at[zz, xx, c], from_sibling.at[zz, xx])
        side_move(zz).start()

    for distance in range(count - 1, 0, -1):
        for kind in (0, 1, 2):
            for up in (True, False):
                target = z + distance if up else z - distance
                exists = target < count if up else target >= 0
                feeds = can_down if up else can_up

                @pl.when(exists)
                def _():
                    mine = half_ref(target, ox if kind == 1 else x, 1 if kind == 2 else 0)
                    if kind == 2:
                        side_move(target).wait_recv()
                        add(mine, from_side.at[1 + target])

                    @pl.when(feeds)
                    def _():
                        back(up, kind, target).wait_recv()
                        add(mine, from_line.at[0 if up else 1, kind, target])

                    back(up, kind, target).start()

    for kind in (1, 0, 2):
        mine = half_ref(z, ox if kind == 1 else x, 1 if kind == 2 else 0)
        if kind == 2:
            side_move(z).wait_recv()
            add(mine, from_side.at[1 + z])
        for up in (True, False):

            @pl.when(can_down if up else can_up)
            def _():
                back(up, kind, z).wait_recv()
                add(mine, from_line.at[0 if up else 1, kind, z])

        if kind == 1:
            last_move().start()

    mixer_move.wait()
    mixer_ref[...] = (
        terms_ref[x, c].astype(F32)
        + mixer_sibling[x].astype(F32)
        + mixer_side[...].astype(F32)
    ).astype(BF16)
    expert_ref[:, half:] = (sums[z, x, c, :, half:].astype(F32) + shared[:, half:]).astype(BF16)
    last_move().wait_recv()
    expert_ref[:, :half] = (
        sums[z, x, c, :, :half].astype(F32) + from_side[0].astype(F32) + shared[:, :half]
    ).astype(BF16)

    for step in range(1, group):
        meta_copy(step).wait_send()
    across(0, z).wait_send()
    last_move().wait_send()
    for zz in range(count):
        across(1, zz).wait_send()
        side_move(zz).wait_send()
        for xx in range(2):
            pair(zz, xx).wait_send()
            for h in range(2):
                share(zz, xx, h).wait_send()
        for kind in range(3):

            @pl.when((zz <= z) & can_up)
            def _():
                line(True, kind, zz).wait_send()

            @pl.when((zz >= z) & can_down)
            def _():
                line(False, kind, zz).wait_send()

            @pl.when(zz > z)
            def _():
                back(True, kind, zz).wait_send()

            @pl.when(zz < z)
            def _():
                back(False, kind, zz).wait_send()


def exchange(terms, normed, meta, shared_parts, routed_parts, capacity):
    tokens, width = normed.shape
    count = lax.axis_size("ep")
    group = count * 4
    hidden = routed_parts[0].shape[1]
    half = width // 2
    batch = 8 if group % 8 == 0 else 4
    dma = pltpu.SemaphoreType.DMA
    vmem = pl.BlockSpec(memory_space=pltpu.VMEM)
    return pl.pallas_call(
        lambda *refs: exchange_kernel(capacity, *refs),
        out_shape=[jax.ShapeDtypeStruct((tokens, width), BF16)] * 2,
        in_specs=[vmem] * 6 + [pl.BlockSpec(memory_space=pl.ANY)] * 3,
        out_specs=[vmem] * 2,
        scratch_shapes=[
            pltpu.VMEM((count, 2, 2, tokens, width), BF16),
            pltpu.VMEM(meta.shape, F32),
            pltpu.VMEM((width, hidden), BF16),
            pltpu.VMEM((width, hidden), BF16),
            pltpu.VMEM((hidden, width), BF16),
            pltpu.VMEM((batch * capacity, width), BF16),
            pltpu.VMEM((tokens, width), F32),
            pltpu.VMEM((count, 2, 2, tokens, width), BF16),
            pltpu.VMEM((count, 2, tokens, width), BF16),
            pltpu.VMEM((1 + count, tokens, half), BF16),
            pltpu.VMEM((2, 3, count, tokens, half), BF16),
            pltpu.VMEM((2, tokens, width), BF16),
            pltpu.VMEM((tokens, width), BF16),
            pltpu.VMEM((tokens, width), BF16),
            dma((5,)),
            dma((group - 1,)),
            dma((group - 1,)),
            dma((2, 3, count)),
            dma((3, count)),
            dma((1 + count,)),
            dma((1 + count,)),
            dma((count, 2, 2)),
            dma((count, 2, 2)),
            dma((3, count)),
            dma((2, 3, count)),
            dma((1 + count,)),
            dma((1 + count,)),
            dma((count, 2)),
            dma((count, 2)),
            dma((3,)),
            dma((3,)),
        ],
        compiler_params=pltpu.CompilerParams(
            collective_id=0, has_side_effects=True, vmem_limit_bytes=60 * 2**20
        ),
        name="exchange",
        cost_estimate=pl.CostEstimate(flops=10**10, bytes_accessed=2 * 10**7, transcendentals=0),
    )(terms.reshape(2, 2, tokens, width), normed, meta, *shared_parts, *routed_parts)


def normalise(expert_input, norm_gain):
    widened = expert_input.astype(F32)
    return (
        widened * lax.rsqrt(jnp.mean(widened * widened, axis=-1, keepdims=True) + 1e-06) * norm_gain
    ).astype(BF16)


def route_table(routes, route_weights, experts):
    tokens = routes.shape[0]
    named = routes[:, None, :] == jnp.arange(experts, dtype=jnp.int32)[None, :, None]
    weight = jnp.sum(jnp.where(named, route_weights[:, None, :], 0.0), axis=2)
    chosen = jnp.any(named, axis=2)
    earlier = jnp.arange(tokens)[None, :] < jnp.arange(tokens)[:, None]
    slot = jnp.dot(earlier.astype(BF16), chosen.astype(BF16), preferred_element_type=F32)
    slot = jnp.where(chosen, slot, -1.0)
    table = jnp.stack([weight.T, slot.T], axis=1)
    return jnp.pad(table, ((0, 0), (0, 6), (0, 0)))


def expert_rows(arrived, gate_weight, up_weight, down_weight):
    sources, capacity, model_width = arrived.shape
    flat_rows = arrived.reshape(sources * capacity, model_width)
    gate_part = jnp.dot(flat_rows, gate_weight[0], preferred_element_type=jnp.float32)
    up_part = jnp.dot(flat_rows, up_weight[0], preferred_element_type=jnp.float32)
    hidden = (jax.nn.silu(gate_part) * up_part).astype(jnp.bfloat16)
    result = jnp.dot(hidden, down_weight[0], preferred_element_type=jnp.float32).astype(
        jnp.bfloat16
    )
    return result.reshape(sources, capacity, model_width)


def experts_half(
    expert_input,
    norm_gain,
    routes,
    route_weights,
    gate_weight,
    up_weight,
    down_weight,
    shared_gate,
    shared_up,
    shared_down,
):
    tokens, top_count = routes.shape
    model_width = expert_input.shape[1]
    ep_count = lax.axis_size("ep")
    tp_count = lax.axis_size("tp")
    experts = ep_count * tp_count
    capacity = max(2, 3 * tokens * top_count // (2 * experts))
    widened = expert_input.astype(jnp.float32)
    normed = (
        widened * lax.rsqrt(jnp.mean(widened * widened, axis=-1, keepdims=True) + 1e-06) * norm_gain
    ).astype(jnp.bfloat16)
    flat_routes = routes.reshape(-1)
    one_hot = (flat_routes[:, None] == jnp.arange(experts, dtype=jnp.int32)[None, :]).astype(
        jnp.int32
    )
    before = jnp.cumsum(one_hot, axis=0) - one_hot
    slot_index = jnp.sum(before * one_hot, axis=1)
    target = flat_routes * capacity + slot_index
    picker = (jnp.arange(experts * capacity, dtype=jnp.int32)[:, None] == target[None, :]).astype(
        jnp.bfloat16
    )
    picker = jnp.sum(picker.reshape(experts * capacity, tokens, top_count), axis=2)
    outgoing = jnp.dot(picker, normed, preferred_element_type=jnp.float32).astype(jnp.bfloat16)
    outgoing = outgoing.reshape(experts, capacity, model_width)
    came_back = lax.all_to_all(
        expert_rows(
            lax.all_to_all(outgoing, ("ep", "tp"), split_axis=0, concat_axis=0, tiled=True),
            gate_weight,
            up_weight,
            down_weight,
        ),
        ("ep", "tp"),
        split_axis=0,
        concat_axis=0,
        tiled=True,
    )
    back_rows = came_back.reshape(experts * capacity, model_width)
    picked = jnp.take(back_rows, target, axis=0).reshape(tokens, top_count, model_width)
    routed = jnp.sum(picked.astype(jnp.float32) * route_weights[:, :, None], axis=1)
    shared_hidden = (
        jax.nn.silu(jnp.dot(normed, shared_gate, preferred_element_type=jnp.float32))
        * jnp.dot(normed, shared_up, preferred_element_type=jnp.float32)
    ).astype(jnp.bfloat16)
    shared_term = jnp.dot(shared_hidden, shared_down, preferred_element_type=jnp.float32)
    return (routed + shared_term).astype(jnp.bfloat16)


def per_device(
    queries,
    key_value,
    key_bias,
    out_weight,
    expert_input,
    norm_gain,
    routes,
    route_weights,
    gate_weight,
    up_weight,
    down_weight,
    shared_gate,
    shared_up,
    shared_down,
):
    terms = project(attend(queries, key_value, key_bias), out_weight)
    tokens, top_count = routes.shape
    width = expert_input.shape[1]
    tp_count = lax.axis_size("tp")
    experts = lax.axis_size("ep") * tp_count
    if tp_count == 4 and experts * tokens * width * 2 <= 8 * 2**20:
        capacity = max(2, 3 * tokens * top_count // (2 * experts))
        mixer_output, expert_output = exchange(
            terms,
            normalise(expert_input, norm_gain),
            route_table(routes, route_weights, experts),
            (shared_gate, shared_up, shared_down),
            (gate_weight[0], up_weight[0], down_weight[0]),
            capacity,
        )
        return (mixer_output, expert_output)
    mixer_output = lax.psum_scatter(terms, "tp", scatter_dimension=0, tiled=True)
    expert_output = experts_half(
        expert_input,
        norm_gain,
        routes,
        route_weights,
        gate_weight,
        up_weight,
        down_weight,
        shared_gate,
        shared_up,
        shared_down,
    )
    return (mixer_output, expert_output)


def solution(mesh):
    placed = (
        P(("grp", "ep"), "tp"),
        P(("grp", "ep"), "tp", None),
        P("tp", ("grp", "ep")),
        P("tp", None),
        P(("grp", "ep", "tp"), None),
        P(),
        P(("grp", "ep", "tp"), None),
        P(("grp", "ep", "tp"), None),
        P(("ep", "tp"), None, None),
        P(("ep", "tp"), None, None),
        P(("ep", "tp"), None, None),
        P(),
        P(),
        P(),
    )
    return jax.shard_map(
        per_device,
        mesh=mesh,
        in_specs=placed,
        out_specs=(P(("grp", "ep", "tp"), None), P(("grp", "ep", "tp"), None)),
        check_vma=False,
    )
```

```python
import jax
import jax.numpy as jnp
from jax import lax
from jax.experimental import pallas as pl
from jax.experimental.pallas import tpu as pltpu
from jax.sharding import PartitionSpec as P

MESH = pl.DeviceIdType.MESH
F32 = jnp.float32
BF16 = jnp.bfloat16


def passed_along(block, axis, distance):
    devices = range(lax.axis_size(axis))
    route = [(i - distance, i) for i in devices if i - distance in devices]
    return lax.ppermute(block, axis, route)


def attention_tile(q, k, v, bias, upper, kept, masked):
    z = lax.dot_general(q, k, (((1,), (1,)), ((), ())), preferred_element_type=F32) * 0.125 + bias
    tail = jnp.log(1.0 + jnp.exp(-jnp.abs(z)))
    log_sig = jnp.minimum(z, 0.0) - tail
    keep = -(jnp.maximum(z, 0.0) + tail)
    if masked:
        rows = lax.broadcasted_iota(jnp.int32, z.shape, 0)
        columns = lax.broadcasted_iota(jnp.int32, z.shape, 1)
        allowed = columns < rows
        keep = jnp.where(allowed, keep, 0.0)
    high = keep.astype(BF16)
    low = (keep - high.astype(F32)).astype(BF16)
    after = jnp.dot(high, upper, preferred_element_type=F32)
    after = after + jnp.dot(low, upper, preferred_element_type=F32)
    weight = jnp.exp(log_sig + after + kept)
    if masked:
        weight = jnp.where(allowed, weight, 0.0)
    part = jnp.dot(weight.astype(BF16), v, preferred_element_type=F32)
    return part, kept + jnp.sum(keep, axis=1, keepdims=True)


def attention_kernel(place_ref, q_ref, kv_ref, bias_ref, out_ref, total, kept):
    span, head_dim = q_ref.shape[1:]
    spans = kv_ref.shape[0]
    size = min(span, 256)
    tiles = span // size
    rows = lax.broadcasted_iota(jnp.int32, (size, size), 0)
    columns = lax.broadcasted_iota(jnp.int32, (size, size), 1)
    upper = jnp.where(rows > columns, 1.0, 0.0).astype(BF16)

    def tile(distance, i, j, masked, state):
        there = pl.ds(j * size, size)
        part, after = attention_tile(
            q_ref[0, i * size : (i + 1) * size, :],
            kv_ref[distance, 0, there, :head_dim],
            kv_ref[distance, 0, there, head_dim:],
            bias_ref[distance, 0, :, there].astype(F32),
            upper,
            state[1],
            masked,
        )
        return state[0] + part, after

    for i in range(tiles):
        state = (jnp.zeros((size, head_dim), F32), jnp.zeros((size, 1), F32))
        for j in range(i, -1, -1):
            state = tile(0, i, j, j == i, state)
        total[i] = state[0]
        kept[i] = jnp.broadcast_to(state[1], kept.shape[1:])
    for distance in range(1, spans):

        @pl.when(distance <= place_ref[0])
        def _():
            for i in range(tiles):
                state = (total[i], kept[i, :, :1])
                for j in range(tiles - 1, -1, -1):
                    state = tile(distance, i, j, False, state)
                total[i] = state[0]
                kept[i] = jnp.broadcast_to(state[1], kept.shape[1:])

    for i in range(tiles):
        out_ref[0, i * size : (i + 1) * size, :] = total[i].astype(out_ref.dtype)


def attend(queries, key_value, key_bias):
    span, key_groups, pair_width = key_value.shape
    head_dim = pair_width // 2
    heads = queries.shape[1] // head_dim
    per_group = heads // key_groups
    axis_size = lax.axis_size("ep")
    chain_length = axis_size // max(1, axis_size // 4)
    place = lax.axis_index("ep")
    chain_place = jnp.minimum((place + 2) % chain_length, place)
    furthest = max(min((p + 2) % chain_length, p) for p in range(axis_size))
    packed = jnp.concatenate([key_value.reshape(-1, pair_width), key_bias.reshape(-1, pair_width)])
    visiting = [packed]
    for _ in range(furthest):
        visiting.append(passed_along(visiting[-1], "ep", 1))
    visiting = jnp.stack(visiting)
    keys = visiting[:, : span * key_groups].reshape(-1, span, key_groups, pair_width)
    keys = keys.transpose(0, 2, 1, 3)
    biases = visiting[:, span * key_groups :].reshape(-1, key_groups, 1, span)
    size = min(span, 256)
    attended = pl.pallas_call(
        attention_kernel,
        grid=(heads,),
        out_shape=jax.ShapeDtypeStruct((heads, span, head_dim), BF16),
        in_specs=[
            pl.BlockSpec(memory_space=pltpu.SMEM),
            pl.BlockSpec((1, span, head_dim), lambda h: (h, 0, 0)),
            pl.BlockSpec((furthest + 1, 1, span, pair_width), lambda h: (0, h // per_group, 0, 0)),
            pl.BlockSpec((furthest + 1, 1, 1, span), lambda h: (0, h // per_group, 0, 0)),
        ],
        out_specs=pl.BlockSpec((1, span, head_dim), lambda h: (h, 0, 0)),
        scratch_shapes=[
            pltpu.VMEM((span // size, size, head_dim), F32),
            pltpu.VMEM((span // size, size, 128), F32),
        ],
        name="attention",
        cost_estimate=pl.CostEstimate(flops=4 * 10**9, bytes_accessed=10**6, transcendentals=0),
    )(
        chain_place.reshape(1),
        queries.reshape(span, heads, head_dim).transpose(1, 0, 2),
        keys,
        biases,
    )
    return attended.transpose(1, 0, 2).reshape(span, heads * head_dim)


def project(attended, out_weight):
    return jnp.dot(attended, out_weight, preferred_element_type=F32).astype(BF16)


def exchange_kernel(
    capacity,
    batch,
    terms_ref,
    normed_ref,
    meta_ref,
    shared_gate,
    shared_up,
    shared_down,
    gate_hbm,
    up_hbm,
    down_hbm,
    mixer_ref,
    expert_ref,
    gathered,
    meta,
    gate_v,
    up_v,
    down_v,
    chosen,
    shared,
    sums,
    from_sibling,
    from_side,
    from_line,
    mixer_sibling,
    mixer_side,
    mixer_sum,
    load_sem,
    meta_send,
    meta_recv,
    zs_send,
    zs_recv,
    x_send,
    x_recv,
    s_send,
    s_recv,
    rz_send,
    rz_recv,
    rx_send,
    rx_recv,
    rs_send,
    rs_recv,
    m_send,
    m_recv,
):
    count = lax.axis_size("ep")
    width = normed_ref.shape[1]
    tokens = normed_ref.shape[0]
    cut = width // 4
    spans = (slice(0, cut), slice(cut, width))
    pieces = (pl.ds(0, cut), pl.ds(cut, width - cut))
    z = lax.axis_index("ep")
    t = lax.axis_index("tp")
    x, c = t // 2, t % 2
    ox, oc = 1 - x, 1 - c
    side, sibling = ox * 2 + c, x * 2 + oc
    group = count * 4
    me = z * 4 + t

    loads = [
        pltpu.make_async_copy(a, b, load_sem.at[i])
        for i, (a, b) in enumerate(((gate_hbm, gate_v), (up_hbm, up_v), (down_hbm, down_v)))
    ]
    own_load = pltpu.make_async_copy(normed_ref, gathered.at[z, x, c], load_sem.at[3])
    own_meta = pltpu.make_async_copy(meta_ref.at[me], meta.at[me], load_sem.at[4])
    own_load.start()
    own_meta.start()

    barrier = pltpu.get_barrier_semaphore()
    for step in range(1, group):
        other = (me + step) % group
        pl.semaphore_signal(
            barrier, 1, device_id={"ep": other // 4, "tp": other % 4}, device_id_type=MESH
        )
    pl.semaphore_wait(barrier, group - 1)

    def copy(src, dst, send, recv, ep, tp):
        return pltpu.make_async_remote_copy(
            src_ref=src,
            dst_ref=dst,
            send_sem=send,
            recv_sem=recv,
            device_id={"ep": ep, "tp": tp},
            device_id_type=MESH,
        )

    own_load.wait()
    own_meta.wait()

    def part(zz, xx, cc, h):
        return gathered.at[zz, xx, cc, :, pieces[h]]

    def line(up, kind, zz):
        block = part(zz, ox if kind == 1 else x, c, 1 if kind == 2 else 0)
        return copy(
            block,
            block,
            zs_send.at[0 if up else 1, kind, zz],
            zs_recv.at[kind, zz],
            z + (1 if up else -1),
            t,
        )

    def across(slot, zz):
        block = part(zz, x, c, 0 if slot == 0 else 1)
        index = 0 if slot == 0 else 1 + zz
        return copy(block, block, x_send.at[index], x_recv.at[index], z, side)

    def across_in(slot, zz):
        block = part(zz, ox, c, 0 if slot == 0 else 1)
        index = 0 if slot == 0 else 1 + zz
        return copy(block, block, x_send.at[index], x_recv.at[index], z, side)

    def share(zz, xx, h):
        block = part(zz, xx, c, h)
        return copy(block, block, s_send.at[zz, xx, h], s_recv.at[zz, xx, h], z, sibling)

    def share_in(zz, xx, h):
        block = part(zz, xx, oc, h)
        return copy(block, block, s_send.at[zz, xx, h], s_recv.at[zz, xx, h], z, sibling)

    def meta_copy(step):
        other = (me + step) % group
        return copy(
            meta_ref.at[other],
            meta.at[me],
            meta_send.at[step - 1],
            meta_recv.at[step - 1],
            other // 4,
            other % 4,
        )

    def meta_in(step):
        other = (me + group - step) % group
        return copy(
            meta_ref.at[other],
            meta.at[other],
            meta_send.at[step - 1],
            meta_recv.at[step - 1],
            other // 4,
            other % 4,
        )

    can_up, can_down = z + 1 < count, z >= 1
    slots = lax.broadcasted_iota(jnp.int32, (capacity, tokens), 0).astype(F32)

    def picker(source):
        return jnp.where(meta[source, 1:2, :] == slots, 1.0, 0.0)

    def rows_of(source):
        return pl.ds(pl.multiple_of(source * capacity, 16), capacity)

    def pick(zz, xx, cc, h):
        source = zz * 4 + xx * 2 + cc
        columns = spans[h]
        chosen[rows_of(source), columns] = jnp.dot(
            picker(source).astype(BF16),
            gathered[zz, xx, cc, :, columns],
            preferred_element_type=F32,
        ).astype(BF16)

    def pick_both(zz, xx, h):
        pick(zz, xx, c, h)
        share_in(zz, xx, h).wait_recv()
        pick(zz, xx, oc, h)

    across(0, z).start()
    for kind in (2, 0):

        @pl.when(can_up)
        def _():
            line(True, kind, z).start()

        @pl.when(can_down)
        def _():
            line(False, kind, z).start()

    across(1, z).start()
    for step in range(1, group):
        meta_copy(step).start()
    share(z, x, 0).start()
    share(z, x, 1).start()
    for load in loads:
        load.start()

    def mixer_pair(xx):
        return copy(
            terms_ref.at[xx, oc],
            mixer_sibling.at[xx],
            m_send.at[xx],
            m_recv.at[xx],
            z,
            sibling,
        )

    for xx in range(2):
        mixer_pair(xx).start()

    hidden_gate = jnp.dot(normed_ref[...], shared_gate[...], preferred_element_type=F32)
    hidden_up = jnp.dot(normed_ref[...], shared_up[...], preferred_element_type=F32)
    shared_hidden = (hidden_gate / (1.0 + jnp.exp(-hidden_gate)) * hidden_up).astype(BF16)
    shared[...] = jnp.dot(shared_hidden, shared_down[...], preferred_element_type=F32)

    across_in(0, z).wait_recv()

    @pl.when(can_up)
    def _():
        line(True, 1, z).start()

    @pl.when(can_down)
    def _():
        line(False, 1, z).start()

    share(z, ox, 0).start()
    for step in range(1, group):
        meta_in(step).wait_recv()
    pick_both(z, x, 0)
    pick_both(z, x, 1)
    pick_both(z, ox, 0)

    def other_side(zz):
        across_in(1, zz).wait_recv()
        share(zz, ox, 1).start()
        pick_both(zz, ox, 1)

    for distance in range(1, count):
        below, above = z - distance, z + distance

        def arrive(kind, zz, going_up, further):
            line(going_up, kind, zz).wait_recv()

            @pl.when(further)
            def _():
                line(going_up, kind, zz).start()

            if kind == 2:
                across(1, zz).start()
            share(zz, ox if kind == 1 else x, 1 if kind == 2 else 0).start()

        for kind in (2, 0, 1):

            @pl.when(below >= 0)
            def _():
                arrive(kind, below, True, can_up)

            @pl.when(above < count)
            def _():
                arrive(kind, above, False, can_down)

            for there, zz in ((below >= 0, below), (above < count, above)):

                @pl.when(there)
                def _():
                    pick_both(zz, ox if kind == 1 else x, 1 if kind == 2 else 0)

        for there, zz in (
            ((z >= 0, z),)
            if distance == 1
            else ((below + 1 >= 0, below + 1), (above - 1 < count, above - 1))
        ):

            @pl.when(there)
            def _():
                other_side(zz)

    for xx in range(2):
        mixer_pair(xx).wait()
    mixer_sum[...] = (
        terms_ref[ox, c].astype(F32) + mixer_sibling[ox].astype(F32)
    ).astype(BF16)
    mixer_move = copy(mixer_sum, mixer_side, m_send.at[2], m_recv.at[2], z, side)
    mixer_move.start()

    for zz in (z - (count - 1), z + (count - 1)):

        @pl.when((zz >= 0) & (zz < count))
        def _():
            other_side(zz)

    for load in loads:
        load.wait()

    @pl.loop(0, group // batch)
    def _(turn):
        block = pl.ds(pl.multiple_of(turn * (batch * capacity), 16), batch * capacity)
        scales = []
        for i in range(batch):
            source = turn * batch + i
            scales.append(
                jnp.sum(picker(source) * meta[source, 0:1, :], axis=1, keepdims=True)
            )
        scale = jnp.concatenate(scales, axis=0)
        gate = jnp.dot(chosen[block, :], gate_v[...], preferred_element_type=F32)
        up = jnp.dot(chosen[block, :], up_v[...], preferred_element_type=F32)
        hidden = (gate / (1.0 + jnp.exp(-gate)) * up).astype(BF16)
        rows = jnp.dot(hidden, down_v[...], preferred_element_type=F32)
        chosen[block, :] = (rows * scale).astype(BF16)

    def spread(zz, xx, cc):
        source = zz * 4 + xx * 2 + cc
        sums[zz, xx, cc] = lax.dot_general(
            picker(source).astype(BF16),
            chosen[rows_of(source), :],
            (((0,), (0,)), ((), ())),
            preferred_element_type=F32,
        ).astype(BF16)

    def pair(zz, xx):
        return copy(
            sums.at[zz, xx, oc],
            from_sibling.at[zz, xx],
            rs_send.at[zz, xx],
            rs_recv.at[zz, xx],
            z,
            sibling,
        )

    def half_ref(zz, xx, h):
        return sums.at[zz, xx, c, :, pieces[h]]

    def side_ref(h, zz):
        return from_side.at[1 + zz] if h else from_side.at[0, :, pieces[0]]

    def line_ref(up, kind, zz):
        slot = from_line.at[0 if up else 1, kind, zz]
        return slot if kind == 2 else slot.at[:, pieces[0]]

    def side_move(zz):
        return copy(
            half_ref(zz, ox, 1), side_ref(1, zz), rx_send.at[1 + zz], rx_recv.at[1 + zz], z, side
        )

    def last_move():
        return copy(half_ref(z, ox, 0), side_ref(0, z), rx_send.at[0], rx_recv.at[0], z, side)

    def back(up, kind, zz):
        return copy(
            half_ref(zz, ox if kind == 1 else x, 1 if kind == 2 else 0),
            line_ref(up, kind, zz),
            rz_send.at[kind, zz],
            rz_recv.at[0 if up else 1, kind, zz],
            z + (1 if up else -1),
            t,
        )

    def add(ref, other):
        ref[...] = (ref[...].astype(F32) + other[...].astype(F32)).astype(BF16)

    order = []
    for k in range(count - 1):
        low = (count - 1 - k) - (z - (count - 1 - k) + count) // count
        high = k + (k - z + count) // count
        order.append(low + (z // (count // 2)) * (high - low))
    order.append(z)

    def finish(zz, own):
        for xx in (ox, x):
            pair(zz, xx).wait_recv()
            add(sums.at[zz, xx, c], from_sibling.at[zz, xx])
        side_move(zz).start()
        if not own:
            for up, edge in ((True, z == 0), (False, z == count - 1)):

                @pl.when(edge)
                def _():
                    back(up, 1, zz).start()
                    back(up, 0, zz).start()

    for k in range(count + 1):
        if k < count:
            for xx in (ox, x):
                spread(order[k], xx, oc)
                pair(order[k], xx).start()
            for xx in (ox, x):
                spread(order[k], xx, c)
        if k >= 1:
            finish(order[k - 1], k == count)

    for distance in range(count - 1, 0, -1):
        for kind in (1, 0, 2):
            for up in (True, False):
                target = z + distance if up else z - distance
                exists = target < count if up else target >= 0
                feeds = can_down if up else can_up

                @pl.when(exists)
                def _():
                    mine = half_ref(target, ox if kind == 1 else x, 1 if kind == 2 else 0)
                    if kind == 2:
                        side_move(target).wait_recv()
                        add(mine, from_side.at[1 + target])

                    @pl.when(feeds)
                    def _():
                        back(up, kind, target).wait_recv()
                        add(mine, line_ref(up, kind, target))
                        if kind != 2:
                            back(up, kind, target).start()

                    if kind == 2:
                        back(up, kind, target).start()

    for kind in (1, 0, 2):
        mine = half_ref(z, ox if kind == 1 else x, 1 if kind == 2 else 0)
        if kind == 2:
            side_move(z).wait_recv()
            add(mine, from_side.at[1 + z])
        for up in (True, False):

            @pl.when(can_down if up else can_up)
            def _():
                back(up, kind, z).wait_recv()
                add(mine, line_ref(up, kind, z))

        if kind == 1:
            last_move().start()

    mixer_move.wait()
    mixer_ref[...] = (
        terms_ref[x, c].astype(F32)
        + mixer_sibling[x].astype(F32)
        + mixer_side[...].astype(F32)
    ).astype(BF16)
    expert_ref[:, cut:] = (sums[z, x, c, :, cut:].astype(F32) + shared[:, cut:]).astype(BF16)
    last_move().wait_recv()
    expert_ref[:, :cut] = (
        sums[z, x, c, :, :cut].astype(F32) + from_side[0, :, :cut].astype(F32) + shared[:, :cut]
    ).astype(BF16)

    for step in range(1, group):
        meta_copy(step).wait_send()
    across(0, z).wait_send()
    last_move().wait_send()
    for zz in range(count):
        across(1, zz).wait_send()
        side_move(zz).wait_send()
        for xx in range(2):
            pair(zz, xx).wait_send()
            for h in range(2):
                share(zz, xx, h).wait_send()
        for kind in range(3):

            @pl.when((zz <= z) & can_up)
            def _():
                line(True, kind, zz).wait_send()

            @pl.when((zz >= z) & can_down)
            def _():
                line(False, kind, zz).wait_send()

            @pl.when(zz > z)
            def _():
                back(True, kind, zz).wait_send()

            @pl.when(zz < z)
            def _():
                back(False, kind, zz).wait_send()


def exchange(terms, normed, meta, shared_parts, routed_parts, capacity):
    tokens, width = normed.shape
    count = lax.axis_size("ep")
    group = count * 4
    hidden = routed_parts[0].shape[1]
    rest = width - width // 4
    batch = 8 if group % 8 == 0 else 4
    dma = pltpu.SemaphoreType.DMA
    vmem = pl.BlockSpec(memory_space=pltpu.VMEM)
    return pl.pallas_call(
        lambda *refs: exchange_kernel(capacity, batch, *refs),
        out_shape=[jax.ShapeDtypeStruct((tokens, width), BF16)] * 2,
        in_specs=[vmem] * 6 + [pl.BlockSpec(memory_space=pl.ANY)] * 3,
        out_specs=[vmem] * 2,
        scratch_shapes=[
            pltpu.VMEM((count, 2, 2, tokens, width), BF16),
            pltpu.VMEM(meta.shape, F32),
            pltpu.VMEM((width, hidden), BF16),
            pltpu.VMEM((width, hidden), BF16),
            pltpu.VMEM((hidden, width), BF16),
            pltpu.VMEM((group * capacity, width), BF16),
            pltpu.VMEM((tokens, width), F32),
            pltpu.VMEM((count, 2, 2, tokens, width), BF16),
            pltpu.VMEM((count, 2, tokens, width), BF16),
            pltpu.VMEM((1 + count, tokens, rest), BF16),
            pltpu.VMEM((2, 3, count, tokens, rest), BF16),
            pltpu.VMEM((2, tokens, width), BF16),
            pltpu.VMEM((tokens, width), BF16),
            pltpu.VMEM((tokens, width), BF16),
            dma((5,)),
            dma((group - 1,)),
            dma((group - 1,)),
            dma((2, 3, count)),
            dma((3, count)),
            dma((1 + count,)),
            dma((1 + count,)),
            dma((count, 2, 2)),
            dma((count, 2, 2)),
            dma((3, count)),
            dma((2, 3, count)),
            dma((1 + count,)),
            dma((1 + count,)),
            dma((count, 2)),
            dma((count, 2)),
            dma((3,)),
            dma((3,)),
        ],
        compiler_params=pltpu.CompilerParams(
            collective_id=0, has_side_effects=True, vmem_limit_bytes=60 * 2**20
        ),
        name="exchange",
        cost_estimate=pl.CostEstimate(flops=10**10, bytes_accessed=2 * 10**7, transcendentals=0),
    )(terms.reshape(2, 2, tokens, width), normed, meta, *shared_parts, *routed_parts)


def normalise(expert_input, norm_gain):
    widened = expert_input.astype(F32)
    return (
        widened * lax.rsqrt(jnp.mean(widened * widened, axis=-1, keepdims=True) + 1e-06) * norm_gain
    ).astype(BF16)


def route_table(routes, route_weights, experts):
    tokens = routes.shape[0]
    named = routes[:, None, :] == jnp.arange(experts, dtype=jnp.int32)[None, :, None]
    weight = jnp.sum(jnp.where(named, route_weights[:, None, :], 0.0), axis=2)
    chosen = jnp.any(named, axis=2)
    earlier = jnp.arange(tokens)[None, :] < jnp.arange(tokens)[:, None]
    slot = jnp.dot(earlier.astype(BF16), chosen.astype(BF16), preferred_element_type=F32)
    slot = jnp.where(chosen, slot, -1.0)
    table = jnp.stack([weight.T, slot.T], axis=1)
    return jnp.pad(table, ((0, 0), (0, 6), (0, 0)))


def expert_rows(arrived, gate_weight, up_weight, down_weight):
    sources, capacity, model_width = arrived.shape
    flat_rows = arrived.reshape(sources * capacity, model_width)
    gate_part = jnp.dot(flat_rows, gate_weight[0], preferred_element_type=jnp.float32)
    up_part = jnp.dot(flat_rows, up_weight[0], preferred_element_type=jnp.float32)
    hidden = (jax.nn.silu(gate_part) * up_part).astype(jnp.bfloat16)
    result = jnp.dot(hidden, down_weight[0], preferred_element_type=jnp.float32).astype(
        jnp.bfloat16
    )
    return result.reshape(sources, capacity, model_width)


def experts_half(
    expert_input,
    norm_gain,
    routes,
    route_weights,
    gate_weight,
    up_weight,
    down_weight,
    shared_gate,
    shared_up,
    shared_down,
):
    tokens, top_count = routes.shape
    model_width = expert_input.shape[1]
    ep_count = lax.axis_size("ep")
    tp_count = lax.axis_size("tp")
    experts = ep_count * tp_count
    capacity = max(2, 3 * tokens * top_count // (2 * experts))
    widened = expert_input.astype(jnp.float32)
    normed = (
        widened * lax.rsqrt(jnp.mean(widened * widened, axis=-1, keepdims=True) + 1e-06) * norm_gain
    ).astype(jnp.bfloat16)
    flat_routes = routes.reshape(-1)
    one_hot = (flat_routes[:, None] == jnp.arange(experts, dtype=jnp.int32)[None, :]).astype(
        jnp.int32
    )
    before = jnp.cumsum(one_hot, axis=0) - one_hot
    slot_index = jnp.sum(before * one_hot, axis=1)
    target = flat_routes * capacity + slot_index
    picker = (jnp.arange(experts * capacity, dtype=jnp.int32)[:, None] == target[None, :]).astype(
        jnp.bfloat16
    )
    picker = jnp.sum(picker.reshape(experts * capacity, tokens, top_count), axis=2)
    outgoing = jnp.dot(picker, normed, preferred_element_type=jnp.float32).astype(jnp.bfloat16)
    outgoing = outgoing.reshape(experts, capacity, model_width)
    came_back = lax.all_to_all(
        expert_rows(
            lax.all_to_all(outgoing, ("ep", "tp"), split_axis=0, concat_axis=0, tiled=True),
            gate_weight,
            up_weight,
            down_weight,
        ),
        ("ep", "tp"),
        split_axis=0,
        concat_axis=0,
        tiled=True,
    )
    back_rows = came_back.reshape(experts * capacity, model_width)
    picked = jnp.take(back_rows, target, axis=0).reshape(tokens, top_count, model_width)
    routed = jnp.sum(picked.astype(jnp.float32) * route_weights[:, :, None], axis=1)
    shared_hidden = (
        jax.nn.silu(jnp.dot(normed, shared_gate, preferred_element_type=jnp.float32))
        * jnp.dot(normed, shared_up, preferred_element_type=jnp.float32)
    ).astype(jnp.bfloat16)
    shared_term = jnp.dot(shared_hidden, shared_down, preferred_element_type=jnp.float32)
    return (routed + shared_term).astype(jnp.bfloat16)


def per_device(
    queries,
    key_value,
    key_bias,
    out_weight,
    expert_input,
    norm_gain,
    routes,
    route_weights,
    gate_weight,
    up_weight,
    down_weight,
    shared_gate,
    shared_up,
    shared_down,
):
    terms = project(attend(queries, key_value, key_bias), out_weight)
    tokens, top_count = routes.shape
    width = expert_input.shape[1]
    tp_count = lax.axis_size("tp")
    experts = lax.axis_size("ep") * tp_count
    capacity = max(2, 3 * tokens * top_count // (2 * experts))
    if tp_count == 4 and capacity % 16 == 0 and experts * tokens * width * 2 <= 8 * 2**20:
        mixer_output, expert_output = exchange(
            terms,
            normalise(expert_input, norm_gain),
            route_table(routes, route_weights, experts),
            (shared_gate, shared_up, shared_down),
            (gate_weight[0], up_weight[0], down_weight[0]),
            capacity,
        )
        return (mixer_output, expert_output)
    mixer_output = lax.psum_scatter(terms, "tp", scatter_dimension=0, tiled=True)
    expert_output = experts_half(
        expert_input,
        norm_gain,
        routes,
        route_weights,
        gate_weight,
        up_weight,
        down_weight,
        shared_gate,
        shared_up,
        shared_down,
    )
    return (mixer_output, expert_output)


def solution(mesh):
    placed = (
        P(("grp", "ep"), "tp"),
        P(("grp", "ep"), "tp", None),
        P("tp", ("grp", "ep")),
        P("tp", None),
        P(("grp", "ep", "tp"), None),
        P(),
        P(("grp", "ep", "tp"), None),
        P(("grp", "ep", "tp"), None),
        P(("ep", "tp"), None, None),
        P(("ep", "tp"), None, None),
        P(("ep", "tp"), None, None),
        P(),
        P(),
        P(),
    )
    return jax.shard_map(
        per_device,
        mesh=mesh,
        in_specs=placed,
        out_specs=(P(("grp", "ep", "tp"), None), P(("grp", "ep", "tp"), None)),
        check_vma=False,
    )
```

```python
import jax
import jax.numpy as jnp
from jax import lax
from jax.experimental import pallas as pl
from jax.experimental.pallas import tpu as pltpu
from jax.sharding import PartitionSpec as P

MESH = pl.DeviceIdType.MESH
F32 = jnp.float32
BF16 = jnp.bfloat16


def passed_along(block, axis, distance):
    devices = range(lax.axis_size(axis))
    route = [(i - distance, i) for i in devices if i - distance in devices]
    return lax.ppermute(block, axis, route)


def attention_tile(q, k, v, bias, upper, kept, masked):
    z = lax.dot_general(q, k, (((1,), (1,)), ((), ())), preferred_element_type=F32) * 0.125 + bias
    tail = jnp.log(1.0 + jnp.exp(-jnp.abs(z)))
    log_sig = jnp.minimum(z, 0.0) - tail
    keep = -(jnp.maximum(z, 0.0) + tail)
    if masked:
        rows = lax.broadcasted_iota(jnp.int32, z.shape, 0)
        columns = lax.broadcasted_iota(jnp.int32, z.shape, 1)
        allowed = columns < rows
        keep = jnp.where(allowed, keep, 0.0)
    high = keep.astype(BF16)
    low = (keep - high.astype(F32)).astype(BF16)
    after = jnp.dot(high, upper, preferred_element_type=F32)
    after = after + jnp.dot(low, upper, preferred_element_type=F32)
    weight = jnp.exp(log_sig + after + kept)
    if masked:
        weight = jnp.where(allowed, weight, 0.0)
    part = jnp.dot(weight.astype(BF16), v, preferred_element_type=F32)
    return part, kept + jnp.sum(keep, axis=1, keepdims=True)


def attention_kernel(place_ref, q_ref, kv_ref, bias_ref, out_ref, total, kept):
    span, head_dim = q_ref.shape[1:]
    spans = kv_ref.shape[0]
    size = min(span, 256)
    tiles = span // size
    rows = lax.broadcasted_iota(jnp.int32, (size, size), 0)
    columns = lax.broadcasted_iota(jnp.int32, (size, size), 1)
    upper = jnp.where(rows > columns, 1.0, 0.0).astype(BF16)

    def tile(distance, i, j, masked, state):
        there = pl.ds(j * size, size)
        part, after = attention_tile(
            q_ref[0, i * size : (i + 1) * size, :],
            kv_ref[distance, 0, there, :head_dim],
            kv_ref[distance, 0, there, head_dim:],
            bias_ref[distance, 0, :, there].astype(F32),
            upper,
            state[1],
            masked,
        )
        return state[0] + part, after

    for i in range(tiles):
        state = (jnp.zeros((size, head_dim), F32), jnp.zeros((size, 1), F32))
        for j in range(i, -1, -1):
            state = tile(0, i, j, j == i, state)
        total[i] = state[0]
        kept[i] = jnp.broadcast_to(state[1], kept.shape[1:])
    for distance in range(1, spans):

        @pl.when(distance <= place_ref[0])
        def _():
            for i in range(tiles):
                state = (total[i], kept[i, :, :1])
                for j in range(tiles - 1, -1, -1):
                    state = tile(distance, i, j, False, state)
                total[i] = state[0]
                kept[i] = jnp.broadcast_to(state[1], kept.shape[1:])

    for i in range(tiles):
        out_ref[0, i * size : (i + 1) * size, :] = total[i].astype(out_ref.dtype)


def attend(queries, key_value, key_bias):
    span, key_groups, pair_width = key_value.shape
    head_dim = pair_width // 2
    heads = queries.shape[1] // head_dim
    per_group = heads // key_groups
    axis_size = lax.axis_size("ep")
    chain_length = axis_size // max(1, axis_size // 4)
    place = lax.axis_index("ep")
    chain_place = jnp.minimum((place + 2) % chain_length, place)
    furthest = max(min((p + 2) % chain_length, p) for p in range(axis_size))
    packed = jnp.concatenate([key_value.reshape(-1, pair_width), key_bias.reshape(-1, pair_width)])
    visiting = [packed]
    for _ in range(furthest):
        visiting.append(passed_along(visiting[-1], "ep", 1))
    visiting = jnp.stack(visiting)
    keys = visiting[:, : span * key_groups].reshape(-1, span, key_groups, pair_width)
    keys = keys.transpose(0, 2, 1, 3)
    biases = visiting[:, span * key_groups :].reshape(-1, key_groups, 1, span)
    size = min(span, 256)
    attended = pl.pallas_call(
        attention_kernel,
        grid=(heads,),
        out_shape=jax.ShapeDtypeStruct((heads, span, head_dim), BF16),
        in_specs=[
            pl.BlockSpec(memory_space=pltpu.SMEM),
            pl.BlockSpec((1, span, head_dim), lambda h: (h, 0, 0)),
            pl.BlockSpec((furthest + 1, 1, span, pair_width), lambda h: (0, h // per_group, 0, 0)),
            pl.BlockSpec((furthest + 1, 1, 1, span), lambda h: (0, h // per_group, 0, 0)),
        ],
        out_specs=pl.BlockSpec((1, span, head_dim), lambda h: (h, 0, 0)),
        scratch_shapes=[
            pltpu.VMEM((span // size, size, head_dim), F32),
            pltpu.VMEM((span // size, size, 128), F32),
        ],
        name="attention",
        cost_estimate=pl.CostEstimate(flops=4 * 10**9, bytes_accessed=10**6, transcendentals=0),
    )(
        chain_place.reshape(1),
        queries.reshape(span, heads, head_dim).transpose(1, 0, 2),
        keys,
        biases,
    )
    return attended.transpose(1, 0, 2).reshape(span, heads * head_dim)


def project(attended, out_weight):
    return jnp.dot(attended, out_weight, preferred_element_type=F32).astype(BF16)


def exchange_kernel(
    capacity,
    batch,
    terms_ref,
    normed_ref,
    meta_ref,
    shared_gate,
    shared_up,
    shared_down,
    gate_hbm,
    up_hbm,
    down_hbm,
    mixer_ref,
    expert_ref,
    gathered,
    meta,
    gate_v,
    up_v,
    down_v,
    chosen,
    shared,
    sums,
    from_sibling,
    from_side,
    from_line,
    mixer_sibling,
    mixer_side,
    mixer_sum,
    load_sem,
    meta_send,
    meta_recv,
    zs_send,
    zs_recv,
    x_send,
    x_recv,
    s_send,
    s_recv,
    rz_send,
    rz_recv,
    rx_send,
    rx_recv,
    rs_send,
    rs_recv,
    m_send,
    m_recv,
):
    count = lax.axis_size("ep")
    width = normed_ref.shape[1]
    tokens = normed_ref.shape[0]
    cut = width // 8
    spans = (slice(0, cut), slice(cut, width))
    pieces = (pl.ds(0, cut), pl.ds(cut, width - cut))
    z = lax.axis_index("ep")
    t = lax.axis_index("tp")
    x, c = t // 2, t % 2
    ox, oc = 1 - x, 1 - c
    side, sibling = ox * 2 + c, x * 2 + oc
    group = count * 4
    me = z * 4 + t

    loads = [
        pltpu.make_async_copy(a, b, load_sem.at[i])
        for i, (a, b) in enumerate(((gate_hbm, gate_v), (up_hbm, up_v), (down_hbm, down_v)))
    ]
    own_load = pltpu.make_async_copy(normed_ref, gathered.at[z, x, c], load_sem.at[3])
    own_meta = pltpu.make_async_copy(meta_ref.at[me], meta.at[me], load_sem.at[4])
    own_load.start()
    own_meta.start()

    barrier = pltpu.get_barrier_semaphore()
    for step in range(1, group):
        other = (me + step) % group
        pl.semaphore_signal(
            barrier, 1, device_id={"ep": other // 4, "tp": other % 4}, device_id_type=MESH
        )
    pl.semaphore_wait(barrier, group - 1)

    def copy(src, dst, send, recv, ep, tp):
        return pltpu.make_async_remote_copy(
            src_ref=src,
            dst_ref=dst,
            send_sem=send,
            recv_sem=recv,
            device_id={"ep": ep, "tp": tp},
            device_id_type=MESH,
        )

    own_load.wait()
    own_meta.wait()

    def part(zz, xx, cc, h):
        return gathered.at[zz, xx, cc, :, pieces[h]]

    def line(up, kind, zz):
        block = part(zz, ox if kind == 1 else x, c, 1 if kind == 2 else 0)
        return copy(
            block,
            block,
            zs_send.at[0 if up else 1, kind, zz],
            zs_recv.at[kind, zz],
            z + (1 if up else -1),
            t,
        )

    def across(slot, zz):
        block = part(zz, x, c, 0 if slot == 0 else 1)
        index = 0 if slot == 0 else 1 + zz
        return copy(block, block, x_send.at[index], x_recv.at[index], z, side)

    def across_in(slot, zz):
        block = part(zz, ox, c, 0 if slot == 0 else 1)
        index = 0 if slot == 0 else 1 + zz
        return copy(block, block, x_send.at[index], x_recv.at[index], z, side)

    def share(zz, xx, h):
        block = part(zz, xx, c, h)
        return copy(block, block, s_send.at[zz, xx, h], s_recv.at[zz, xx, h], z, sibling)

    def share_in(zz, xx, h):
        block = part(zz, xx, oc, h)
        return copy(block, block, s_send.at[zz, xx, h], s_recv.at[zz, xx, h], z, sibling)

    def meta_copy(step):
        other = (me + step) % group
        return copy(
            meta_ref.at[other],
            meta.at[me],
            meta_send.at[step - 1],
            meta_recv.at[step - 1],
            other // 4,
            other % 4,
        )

    def meta_in(step):
        other = (me + group - step) % group
        return copy(
            meta_ref.at[other],
            meta.at[other],
            meta_send.at[step - 1],
            meta_recv.at[step - 1],
            other // 4,
            other % 4,
        )

    can_up, can_down = z + 1 < count, z >= 1
    slots = lax.broadcasted_iota(jnp.int32, (capacity, tokens), 0).astype(F32)

    def picker(source):
        return jnp.where(meta[source, 1:2, :] == slots, 1.0, 0.0)

    def rows_of(source):
        return pl.ds(pl.multiple_of(source * capacity, 16), capacity)

    def pick(zz, xx, cc, h):
        source = zz * 4 + xx * 2 + cc
        columns = spans[h]
        chosen[rows_of(source), columns] = jnp.dot(
            picker(source).astype(BF16),
            gathered[zz, xx, cc, :, columns],
            preferred_element_type=F32,
        ).astype(BF16)

    def pick_both(zz, xx, h):
        pick(zz, xx, c, h)
        share_in(zz, xx, h).wait_recv()
        pick(zz, xx, oc, h)

    across(0, z).start()
    for kind in (2, 0):

        @pl.when(can_up)
        def _():
            line(True, kind, z).start()

        @pl.when(can_down)
        def _():
            line(False, kind, z).start()

    across(1, z).start()
    for step in range(1, group):
        meta_copy(step).start()
    share(z, x, 0).start()
    share(z, x, 1).start()
    for load in loads:
        load.start()

    def mixer_pair(xx):
        return copy(
            terms_ref.at[xx, oc],
            mixer_sibling.at[xx],
            m_send.at[xx],
            m_recv.at[xx],
            z,
            sibling,
        )

    for xx in range(2):
        mixer_pair(xx).start()

    hidden_gate = jnp.dot(normed_ref[...], shared_gate[...], preferred_element_type=F32)
    hidden_up = jnp.dot(normed_ref[...], shared_up[...], preferred_element_type=F32)
    shared_hidden = (hidden_gate / (1.0 + jnp.exp(-hidden_gate)) * hidden_up).astype(BF16)
    shared[...] = jnp.dot(shared_hidden, shared_down[...], preferred_element_type=F32)

    across_in(0, z).wait_recv()

    @pl.when(can_up)
    def _():
        line(True, 1, z).start()

    @pl.when(can_down)
    def _():
        line(False, 1, z).start()

    share(z, ox, 0).start()
    for step in range(1, group):
        meta_in(step).wait_recv()
    pick_both(z, x, 0)
    pick_both(z, x, 1)
    pick_both(z, ox, 0)

    def other_side(zz):
        across_in(1, zz).wait_recv()
        share(zz, ox, 1).start()
        pick_both(zz, ox, 1)

    for distance in range(1, count):
        below, above = z - distance, z + distance

        def arrive(kind, zz, going_up, further):
            line(going_up, kind, zz).wait_recv()

            @pl.when(further)
            def _():
                line(going_up, kind, zz).start()

            if kind == 2:
                across(1, zz).start()
            share(zz, ox if kind == 1 else x, 1 if kind == 2 else 0).start()

        for kind in (2, 0, 1):

            @pl.when(below >= 0)
            def _():
                arrive(kind, below, True, can_up)

            @pl.when(above < count)
            def _():
                arrive(kind, above, False, can_down)

            for there, zz in ((below >= 0, below), (above < count, above)):

                @pl.when(there)
                def _():
                    pick_both(zz, ox if kind == 1 else x, 1 if kind == 2 else 0)

        for there, zz in (
            ((z >= 0, z),)
            if distance == 1
            else ((below + 1 >= 0, below + 1), (above - 1 < count, above - 1))
        ):

            @pl.when(there)
            def _():
                other_side(zz)

    for xx in range(2):
        mixer_pair(xx).wait()
    mixer_sum[...] = (
        terms_ref[ox, c].astype(F32) + mixer_sibling[ox].astype(F32)
    ).astype(BF16)
    mixer_move = copy(mixer_sum, mixer_side, m_send.at[2], m_recv.at[2], z, side)
    mixer_move.start()

    for zz in (z - (count - 1), z + (count - 1)):

        @pl.when((zz >= 0) & (zz < count))
        def _():
            other_side(zz)

    for load in loads:
        load.wait()

    @pl.loop(0, group // batch)
    def _(turn):
        block = pl.ds(pl.multiple_of(turn * (batch * capacity), 16), batch * capacity)
        scales = []
        for i in range(batch):
            source = turn * batch + i
            scales.append(
                jnp.sum(picker(source) * meta[source, 0:1, :], axis=1, keepdims=True)
            )
        scale = jnp.concatenate(scales, axis=0)
        gate = jnp.dot(chosen[block, :], gate_v[...], preferred_element_type=F32)
        up = jnp.dot(chosen[block, :], up_v[...], preferred_element_type=F32)
        hidden = (gate / (1.0 + jnp.exp(-gate)) * up).astype(BF16)
        rows = jnp.dot(hidden, down_v[...], preferred_element_type=F32)
        chosen[block, :] = (rows * scale).astype(BF16)

    def spread(zz, xx, cc):
        source = zz * 4 + xx * 2 + cc
        sums[zz, xx, cc] = lax.dot_general(
            picker(source).astype(BF16),
            chosen[rows_of(source), :],
            (((0,), (0,)), ((), ())),
            preferred_element_type=F32,
        ).astype(BF16)

    def pair(zz, xx):
        return copy(
            sums.at[zz, xx, oc],
            from_sibling.at[zz, xx],
            rs_send.at[zz, xx],
            rs_recv.at[zz, xx],
            z,
            sibling,
        )

    def half_ref(zz, xx, h):
        return sums.at[zz, xx, c, :, pieces[h]]

    def side_ref(h, zz):
        return from_side.at[1 + zz] if h else from_side.at[0, :, pieces[0]]

    def line_ref(up, kind, zz):
        slot = from_line.at[0 if up else 1, kind, zz]
        return slot if kind == 2 else slot.at[:, pieces[0]]

    def side_move(zz):
        return copy(
            half_ref(zz, ox, 1), side_ref(1, zz), rx_send.at[1 + zz], rx_recv.at[1 + zz], z, side
        )

    def last_move():
        return copy(half_ref(z, ox, 0), side_ref(0, z), rx_send.at[0], rx_recv.at[0], z, side)

    def back(up, kind, zz):
        return copy(
            half_ref(zz, ox if kind == 1 else x, 1 if kind == 2 else 0),
            line_ref(up, kind, zz),
            rz_send.at[kind, zz],
            rz_recv.at[0 if up else 1, kind, zz],
            z + (1 if up else -1),
            t,
        )

    def add(ref, other):
        ref[...] = (ref[...].astype(F32) + other[...].astype(F32)).astype(BF16)

    order = []
    for k in range(count - 1):
        low = (count - 1 - k) - (z - (count - 1 - k) + count) // count
        high = k + (k - z + count) // count
        order.append(low + (z // (count // 2)) * (high - low))
    order.append(z)

    def finish(zz, own):
        for xx in (ox, x):
            pair(zz, xx).wait_recv()
            add(sums.at[zz, xx, c], from_sibling.at[zz, xx])
        side_move(zz).start()
        if not own:
            for up, edge in ((True, z == 0), (False, z == count - 1)):

                @pl.when(edge)
                def _():
                    back(up, 1, zz).start()
                    back(up, 0, zz).start()

    for k in range(count + 1):
        if k < count:
            for xx in (ox, x):
                spread(order[k], xx, oc)
                pair(order[k], xx).start()
            for xx in (ox, x):
                spread(order[k], xx, c)
        if k >= 1:
            finish(order[k - 1], k == count)

    for distance in range(count - 1, 0, -1):
        for kind in (1, 0, 2):
            for up in (True, False):
                target = z + distance if up else z - distance
                exists = target < count if up else target >= 0
                feeds = can_down if up else can_up

                @pl.when(exists)
                def _():
                    mine = half_ref(target, ox if kind == 1 else x, 1 if kind == 2 else 0)
                    if kind == 2:
                        side_move(target).wait_recv()
                        add(mine, from_side.at[1 + target])

                    @pl.when(feeds)
                    def _():
                        back(up, kind, target).wait_recv()
                        add(mine, line_ref(up, kind, target))
                        if kind != 2:
                            back(up, kind, target).start()

                    if kind == 2:
                        back(up, kind, target).start()

    for kind in (1, 0, 2):
        mine = half_ref(z, ox if kind == 1 else x, 1 if kind == 2 else 0)
        if kind == 2:
            side_move(z).wait_recv()
            add(mine, from_side.at[1 + z])
        for up in (True, False):

            @pl.when(can_down if up else can_up)
            def _():
                back(up, kind, z).wait_recv()
                add(mine, line_ref(up, kind, z))

        if kind == 1:
            last_move().start()

    mixer_move.wait()
    mixer_ref[...] = (
        terms_ref[x, c].astype(F32)
        + mixer_sibling[x].astype(F32)
        + mixer_side[...].astype(F32)
    ).astype(BF16)
    expert_ref[:, cut:] = (sums[z, x, c, :, cut:].astype(F32) + shared[:, cut:]).astype(BF16)
    last_move().wait_recv()
    expert_ref[:, :cut] = (
        sums[z, x, c, :, :cut].astype(F32) + from_side[0, :, :cut].astype(F32) + shared[:, :cut]
    ).astype(BF16)

    for step in range(1, group):
        meta_copy(step).wait_send()
    across(0, z).wait_send()
    last_move().wait_send()
    for zz in range(count):
        across(1, zz).wait_send()
        side_move(zz).wait_send()
        for xx in range(2):
            pair(zz, xx).wait_send()
            for h in range(2):
                share(zz, xx, h).wait_send()
        for kind in range(3):

            @pl.when((zz <= z) & can_up)
            def _():
                line(True, kind, zz).wait_send()

            @pl.when((zz >= z) & can_down)
            def _():
                line(False, kind, zz).wait_send()

            @pl.when(zz > z)
            def _():
                back(True, kind, zz).wait_send()

            @pl.when(zz < z)
            def _():
                back(False, kind, zz).wait_send()


def exchange(terms, normed, meta, shared_parts, routed_parts, capacity):
    tokens, width = normed.shape
    count = lax.axis_size("ep")
    group = count * 4
    hidden = routed_parts[0].shape[1]
    rest = width - width // 8
    batch = 8 if group % 8 == 0 else 4
    dma = pltpu.SemaphoreType.DMA
    vmem = pl.BlockSpec(memory_space=pltpu.VMEM)
    return pl.pallas_call(
        lambda *refs: exchange_kernel(capacity, batch, *refs),
        out_shape=[jax.ShapeDtypeStruct((tokens, width), BF16)] * 2,
        in_specs=[vmem] * 6 + [pl.BlockSpec(memory_space=pl.ANY)] * 3,
        out_specs=[vmem] * 2,
        scratch_shapes=[
            pltpu.VMEM((count, 2, 2, tokens, width), BF16),
            pltpu.VMEM(meta.shape, F32),
            pltpu.VMEM((width, hidden), BF16),
            pltpu.VMEM((width, hidden), BF16),
            pltpu.VMEM((hidden, width), BF16),
            pltpu.VMEM((group * capacity, width), BF16),
            pltpu.VMEM((tokens, width), F32),
            pltpu.VMEM((count, 2, 2, tokens, width), BF16),
            pltpu.VMEM((count, 2, tokens, width), BF16),
            pltpu.VMEM((1 + count, tokens, rest), BF16),
            pltpu.VMEM((2, 3, count, tokens, rest), BF16),
            pltpu.VMEM((2, tokens, width), BF16),
            pltpu.VMEM((tokens, width), BF16),
            pltpu.VMEM((tokens, width), BF16),
            dma((5,)),
            dma((group - 1,)),
            dma((group - 1,)),
            dma((2, 3, count)),
            dma((3, count)),
            dma((1 + count,)),
            dma((1 + count,)),
            dma((count, 2, 2)),
            dma((count, 2, 2)),
            dma((3, count)),
            dma((2, 3, count)),
            dma((1 + count,)),
            dma((1 + count,)),
            dma((count, 2)),
            dma((count, 2)),
            dma((3,)),
            dma((3,)),
        ],
        compiler_params=pltpu.CompilerParams(
            collective_id=0, has_side_effects=True, vmem_limit_bytes=60 * 2**20
        ),
        name="exchange",
        cost_estimate=pl.CostEstimate(flops=10**10, bytes_accessed=2 * 10**7, transcendentals=0),
    )(terms.reshape(2, 2, tokens, width), normed, meta, *shared_parts, *routed_parts)


def normalise(expert_input, norm_gain):
    widened = expert_input.astype(F32)
    return (
        widened * lax.rsqrt(jnp.mean(widened * widened, axis=-1, keepdims=True) + 1e-06) * norm_gain
    ).astype(BF16)


def route_table(routes, route_weights, experts):
    tokens = routes.shape[0]
    named = routes[:, None, :] == jnp.arange(experts, dtype=jnp.int32)[None, :, None]
    weight = jnp.sum(jnp.where(named, route_weights[:, None, :], 0.0), axis=2)
    chosen = jnp.any(named, axis=2)
    earlier = jnp.arange(tokens)[None, :] < jnp.arange(tokens)[:, None]
    slot = jnp.dot(earlier.astype(BF16), chosen.astype(BF16), preferred_element_type=F32)
    slot = jnp.where(chosen, slot, -1.0)
    table = jnp.stack([weight.T, slot.T], axis=1)
    return jnp.pad(table, ((0, 0), (0, 6), (0, 0)))


def expert_rows(arrived, gate_weight, up_weight, down_weight):
    sources, capacity, model_width = arrived.shape
    flat_rows = arrived.reshape(sources * capacity, model_width)
    gate_part = jnp.dot(flat_rows, gate_weight[0], preferred_element_type=jnp.float32)
    up_part = jnp.dot(flat_rows, up_weight[0], preferred_element_type=jnp.float32)
    hidden = (jax.nn.silu(gate_part) * up_part).astype(jnp.bfloat16)
    result = jnp.dot(hidden, down_weight[0], preferred_element_type=jnp.float32).astype(
        jnp.bfloat16
    )
    return result.reshape(sources, capacity, model_width)


def experts_half(
    expert_input,
    norm_gain,
    routes,
    route_weights,
    gate_weight,
    up_weight,
    down_weight,
    shared_gate,
    shared_up,
    shared_down,
):
    tokens, top_count = routes.shape
    model_width = expert_input.shape[1]
    ep_count = lax.axis_size("ep")
    tp_count = lax.axis_size("tp")
    experts = ep_count * tp_count
    capacity = max(2, 3 * tokens * top_count // (2 * experts))
    widened = expert_input.astype(jnp.float32)
    normed = (
        widened * lax.rsqrt(jnp.mean(widened * widened, axis=-1, keepdims=True) + 1e-06) * norm_gain
    ).astype(jnp.bfloat16)
    flat_routes = routes.reshape(-1)
    one_hot = (flat_routes[:, None] == jnp.arange(experts, dtype=jnp.int32)[None, :]).astype(
        jnp.int32
    )
    before = jnp.cumsum(one_hot, axis=0) - one_hot
    slot_index = jnp.sum(before * one_hot, axis=1)
    target = flat_routes * capacity + slot_index
    picker = (jnp.arange(experts * capacity, dtype=jnp.int32)[:, None] == target[None, :]).astype(
        jnp.bfloat16
    )
    picker = jnp.sum(picker.reshape(experts * capacity, tokens, top_count), axis=2)
    outgoing = jnp.dot(picker, normed, preferred_element_type=jnp.float32).astype(jnp.bfloat16)
    outgoing = outgoing.reshape(experts, capacity, model_width)
    came_back = lax.all_to_all(
        expert_rows(
            lax.all_to_all(outgoing, ("ep", "tp"), split_axis=0, concat_axis=0, tiled=True),
            gate_weight,
            up_weight,
            down_weight,
        ),
        ("ep", "tp"),
        split_axis=0,
        concat_axis=0,
        tiled=True,
    )
    back_rows = came_back.reshape(experts * capacity, model_width)
    picked = jnp.take(back_rows, target, axis=0).reshape(tokens, top_count, model_width)
    routed = jnp.sum(picked.astype(jnp.float32) * route_weights[:, :, None], axis=1)
    shared_hidden = (
        jax.nn.silu(jnp.dot(normed, shared_gate, preferred_element_type=jnp.float32))
        * jnp.dot(normed, shared_up, preferred_element_type=jnp.float32)
    ).astype(jnp.bfloat16)
    shared_term = jnp.dot(shared_hidden, shared_down, preferred_element_type=jnp.float32)
    return (routed + shared_term).astype(jnp.bfloat16)


def per_device(
    queries,
    key_value,
    key_bias,
    out_weight,
    expert_input,
    norm_gain,
    routes,
    route_weights,
    gate_weight,
    up_weight,
    down_weight,
    shared_gate,
    shared_up,
    shared_down,
):
    terms = project(attend(queries, key_value, key_bias), out_weight)
    tokens, top_count = routes.shape
    width = expert_input.shape[1]
    tp_count = lax.axis_size("tp")
    experts = lax.axis_size("ep") * tp_count
    capacity = max(2, 3 * tokens * top_count // (2 * experts))
    if tp_count == 4 and capacity % 16 == 0 and experts * tokens * width * 2 <= 8 * 2**20:
        mixer_output, expert_output = exchange(
            terms,
            normalise(expert_input, norm_gain),
            route_table(routes, route_weights, experts),
            (shared_gate, shared_up, shared_down),
            (gate_weight[0], up_weight[0], down_weight[0]),
            capacity,
        )
        return (mixer_output, expert_output)
    mixer_output = lax.psum_scatter(terms, "tp", scatter_dimension=0, tiled=True)
    expert_output = experts_half(
        expert_input,
        norm_gain,
        routes,
        route_weights,
        gate_weight,
        up_weight,
        down_weight,
        shared_gate,
        shared_up,
        shared_down,
    )
    return (mixer_output, expert_output)


def solution(mesh):
    placed = (
        P(("grp", "ep"), "tp"),
        P(("grp", "ep"), "tp", None),
        P("tp", ("grp", "ep")),
        P("tp", None),
        P(("grp", "ep", "tp"), None),
        P(),
        P(("grp", "ep", "tp"), None),
        P(("grp", "ep", "tp"), None),
        P(("ep", "tp"), None, None),
        P(("ep", "tp"), None, None),
        P(("ep", "tp"), None, None),
        P(),
        P(),
        P(),
    )
    return jax.shard_map(
        per_device,
        mesh=mesh,
        in_specs=placed,
        out_specs=(P(("grp", "ep", "tp"), None), P(("grp", "ep", "tp"), None)),
        check_vma=False,
    )
```
